512 devices in a mesh: fs: 128 (over z, x, core), tp: 4 (over y).
Axes of the slice: x: 4, y: 4, z: 16, core: 2. Of those that a mesh axis runs over, the one named last changes fastest.
Arguments:
- tokens: bfloat16 [1024, 2048], P(('fs', 'tp')), may hold values from -6 to 6
- route_experts: int32 [1024, 2], P(('fs', 'tp')), may hold values from 0 to 3, as said below
- route_logits: float32 [1024, 2], P(('fs', 'tp')), may hold values from -8 to 8
- norm_gain: float32 [2048], P('fs'), may hold values from 0.1 to 1.9
- gate_train: float32 [4, 2048, 8192], P(None, 'fs', 'tp'), may hold values from -0.125 to 0.125
- up_train: float32 [4, 2048, 8192], P(None, 'fs', 'tp'), may hold values from -0.125 to 0.125
- down_train: float32 [4, 2048, 8192], P(None, 'fs', 'tp'), may hold values from -0.125 to 0.125
Outputs:
- gate_serve: bfloat16 [128, 2048, 256], P('fs')
- up_serve: bfloat16 [128, 2048, 256], P('fs')
- down_serve: bfloat16 [128, 2048, 256], P('fs')
- mixed: bfloat16 [1024, 2048], P(('fs', 'tp'))
The draws below stay inside these ranges and needn't reach their ends.
Inputs may be any that keep to these rules, and one draw needn't show every extreme that they name: `route_experts`: the two experts of a row differ; any expert may be named by every row of the devices that share one index along tp, and in every draw some expert is.
All inputs are finite; a program needn't handle non-finite values.
Results may differ from the reference program's by a relative error of at most 0.0085.
Values may be sent and summed in bfloat16 or wider, within the bound.
No kernel may reach another device: no remote copies, remote signals or barrier semaphores. Data moves between devices by JAX's collectives and lax.ppermute only.
A program may use at most 64 MiB of HBM per device.

```python
import jax
import jax.numpy as jnp
from jax import lax

D = 2048
FF = 8192
EXPERTS = 4
TOK_DEV = 2
TOKENS = 1024
SLICES = 32
N_TP = 4


def draw_route_experts(key, part):
    keys = jax.random.split(key, 7)
    positions = jnp.arange(TOKENS, dtype=jnp.int32)
    group_index = positions // TOK_DEV % N_TP
    favour = jax.random.randint(keys[0], (N_TP,), 0, EXPERTS, dtype=jnp.int32)
    full_group = jax.random.randint(keys[1], (), 0, N_TP, dtype=jnp.int32)
    share = jax.random.randint(keys[2], (N_TP,), 40, 91, dtype=jnp.int32)
    share = jnp.where(jnp.arange(N_TP, dtype=jnp.int32) == full_group, 100, share)
    picked = jax.random.randint(keys[3], (TOKENS,), 0, 100, dtype=jnp.int32)
    others = jax.random.randint(keys[4], (TOKENS,), 0, EXPERTS, dtype=jnp.int32)
    first = jnp.where(picked < share[group_index], favour[group_index], others)
    offset = jax.random.randint(keys[5], (TOKENS,), 1, EXPERTS, dtype=jnp.int32)
    second = (first + offset) % EXPERTS
    flipped = jax.random.randint(keys[6], (TOKENS,), 0, 2, dtype=jnp.int32)
    column_a = jnp.where(flipped == 1, second, first)
    column_b = jnp.where(flipped == 1, first, second)
    return jnp.stack([column_a, column_b], axis=1).astype(jnp.int32)


def block_scale(stream_key, shape, pieces, low, largest):
    loudness = 1.0
    for position, parts in pieces:
        heights = jax.random.uniform(jax.random.fold_in(jax.random.fold_in(stream_key, 6), position), (parts,), jnp.float32, low / len(pieces), largest / len(pieces))
        loudness = loudness * jnp.repeat(jnp.exp(heights), shape[position] // parts).reshape((-1,) + (1,) * (len(shape) - 1 - position))
    return loudness


def scatter_about(stream_key, dims, scale, most, cuts=(), kind=jnp.bfloat16):
    gain = block_scale(stream_key, dims, cuts, -0.22, 0.18) if cuts else 1.0
    array = jax.random.normal(stream_key, dims, jnp.float32) * scale * gain
    return jnp.minimum(jnp.maximum(array, -most), most).astype(kind)


def setup_inputs(seed: int = 0) -> dict:
    streams_of = jax.random.split(jax.random.key(seed), 8)
    tokens = scatter_about(streams_of[0], (TOKENS, D), 1.0, 6.0, ((0, 512),))
    route_experts = draw_route_experts(jax.random.fold_in(streams_of[7], 71), 0)
    route_logits = scatter_about(streams_of[2], (TOKENS, 2), 2.0, 8.0, ((0, 512),), jnp.float32)
    norm_gain = jnp.clip(1.0 + 0.18 * jax.random.normal(streams_of[3], (D,), jnp.float32), 0.1, 1.9)
    gate_train = scatter_about(streams_of[4], (EXPERTS, D, FF), D ** -0.5, 0.125, ((1, 128), (2, 4)), jnp.float32)
    up_train = scatter_about(streams_of[5], (EXPERTS, D, FF), D ** -0.5, 0.125, ((1, 128), (2, 4)), jnp.float32)
    down_train = scatter_about(streams_of[6], (EXPERTS, D, FF), (FF // 4) ** -0.5, 0.125, ((1, 128), (2, 4)), jnp.float32)
    return {"tokens": tokens, "route_experts": route_experts, "route_logits": route_logits, "norm_gain": norm_gain, "gate_train": gate_train, "up_train": up_train, "down_train": down_train}


def relayout(matrix):
    count, width, hidden = matrix.shape
    blocks = matrix.reshape(count, width, SLICES, hidden // SLICES)
    return blocks.transpose(0, 2, 1, 3).reshape(count * SLICES, width, hidden // SLICES)

def normalize(tokens):
    values = tokens.astype(jnp.float32)
    row_mean = lax.optimization_barrier(jnp.mean(values, axis=-1, keepdims=True))
    centered = values - row_mean
    row_var = lax.optimization_barrier(jnp.mean(centered * centered, axis=-1, keepdims=True))
    return (centered * lax.rsqrt(row_var + 1e-05)).astype(jnp.bfloat16)

def route_table(route_experts, route_logits):
    first = jax.nn.sigmoid(route_logits[:, 0] - route_logits[:, 1])
    second = jax.nn.sigmoid(route_logits[:, 1] - route_logits[:, 0])
    labels = jnp.arange(EXPERTS, dtype=jnp.int32)
    table = first[:, None] * (route_experts[:, 0:1] == labels[None, :]).astype(jnp.float32)
    table = table + second[:, None] * (route_experts[:, 1:2] == labels[None, :]).astype(jnp.float32)
    return table.astype(jnp.bfloat16)

def reference(tokens, route_experts, route_logits, norm_gain, gate_train, up_train, down_train):
    gate_new = (norm_gain[None, :, None] * gate_train).astype(jnp.bfloat16)
    up_new = (norm_gain[None, :, None] * up_train).astype(jnp.bfloat16)
    down_new = down_train.astype(jnp.bfloat16)
    normed = normalize(tokens)
    table = route_table(route_experts, route_logits)
    total = jnp.zeros((tokens.shape[0], tokens.shape[1]), jnp.float32)
    for expert in range(EXPERTS):
        gate_act = jnp.dot(normed, gate_new[expert], preferred_element_type=jnp.float32)
        up_act = jnp.dot(normed, up_new[expert], preferred_element_type=jnp.float32)
        weight = table[:, expert].astype(jnp.float32)[:, None]
        hidden = (weight * jax.nn.silu(gate_act) * up_act).astype(jnp.bfloat16)
        total = total + jnp.dot(hidden, down_new[expert].T, preferred_element_type=jnp.float32)
    return (relayout(gate_new), relayout(up_new), relayout(down_new), total.astype(jnp.bfloat16))
```

```python
import jax
import jax.numpy as jnp
from jax import lax
from jax.sharding import Mesh
from jax.sharding import PartitionSpec as P

FS = ("z", "x", "c")
FS_TP = ("z", "x", "c", "y")
NZ, NX, NC, NY = 16, 4, 2, 4
PAD = 128


def normalize(tokens):
    values = tokens.astype(jnp.float32)
    row_mean = jnp.mean(values, axis=-1, keepdims=True)
    centered = values - row_mean
    row_var = jnp.mean(centered * centered, axis=-1, keepdims=True)
    return (centered * lax.rsqrt(row_var + 1e-05)).astype(jnp.bfloat16)


def route_table(route_experts, route_logits, count):
    first = jax.nn.sigmoid(route_logits[:, 0] - route_logits[:, 1])
    second = jax.nn.sigmoid(route_logits[:, 1] - route_logits[:, 0])
    labels = jnp.arange(count, dtype=jnp.int32)
    table = first[:, None] * (route_experts[:, 0:1] == labels[None, :]).astype(jnp.float32)
    table = table + second[:, None] * (route_experts[:, 1:2] == labels[None, :]).astype(jnp.float32)
    return table.astype(jnp.bfloat16)


def shift(array, axis, by, size):
    return lax.ppermute(array, axis, [(i, (i + by) % size) for i in range(size)])


def ring_parts(own):
    half = own.shape[0] // 2
    below = shift(own, "y", 1, NY)
    above = shift(own, "y", -1, NY)
    far_a = shift(below[:half], "y", 1, NY)
    far_b = shift(above[half:], "y", -1, NY)
    return own, below, jnp.concatenate([far_a, far_b], axis=0), above


def assemble(parts):
    me = lax.axis_index("y")
    rows = []
    for q in range(NY):
        k = (me - q) % NY
        block = parts[0]
        for j in range(1, NY):
            block = jnp.where(k == j, parts[j], block)
        rows.append(block)
    full = jnp.stack(rows, axis=1)
    return full.reshape(1, -1, parts[0].shape[-1])


def per_device(tokens, route_experts, route_logits, norm_gain, gate_train, up_train, down_train):
    experts, depth, wide = gate_train.shape
    r = depth // NY
    block = wide // (NX * NC)
    scale = norm_gain[None, :, None]
    local = jnp.stack([scale * gate_train, scale * up_train, down_train]).astype(jnp.bfloat16)
    local = local.reshape(3, experts, NY, r, NX * NC, block).transpose(4, 2, 0, 1, 3, 5)
    local = local.reshape(NX * NC * NY, 3 * experts, r, block)

    normed = normalize(tokens)
    table = route_table(route_experts, route_logits, experts)
    packed = jnp.concatenate(
        [normed, jnp.pad(table, ((0, 0), (0, PAD - experts)))], axis=1
    )

    swapped = lax.all_to_all(local, ("x", "c", "y"), 0, 0, tiled=True)
    rows_z = lax.all_gather(packed, "z", axis=0, tiled=False)

    swapped = swapped.reshape(NX * NC, NY, 3, experts, r, block).transpose(3, 1, 2, 0, 4, 5)
    swapped = swapped.reshape(NZ, 3, NX * NC, r, block)
    first = lax.all_to_all(swapped[:, :2], "z", 0, 0, tiled=True)
    rows_x = lax.all_gather(rows_z, "x", axis=0, tiled=False)
    rows_c = lax.ppermute(rows_x, "c", [(0, 1), (1, 0)])
    second = lax.all_to_all(swapped[:, 2:], "z", 0, 0, tiled=True)

    gate_own = first[:, 0].reshape(NZ * NX * NC, r, block)
    up_own = first[:, 1].reshape(NZ * NX * NC, r, block)
    down_own = second[:, 0].reshape(NZ * NX * NC, r, block)
    gate_serve = assemble(ring_parts(gate_own))
    up_serve = assemble(ring_parts(up_own))
    down_serve = assemble(ring_parts(down_own))

    width = tokens.shape[1]
    everything = jnp.concatenate([rows_x[None], rows_c[None]], axis=0).reshape(-1, width + PAD)
    rows_all = everything[:, :width]
    table_all = everything[:, width : width + experts]
    own_expert = lax.axis_index("z") // (NZ // experts)
    selector = (jnp.arange(experts, dtype=jnp.int32) == own_expert).astype(jnp.float32)
    weight = jnp.sum(table_all.astype(jnp.float32) * selector[None, :], axis=1)
    gate_act = jnp.dot(rows_all, gate_serve[0], preferred_element_type=jnp.float32)
    up_act = jnp.dot(rows_all, up_serve[0], preferred_element_type=jnp.float32)
    hidden = (weight[:, None] * jax.nn.silu(gate_act) * up_act).astype(jnp.bfloat16)
    half = hidden.shape[0] // 2
    dims = (((1,), (1,)), ((), ()))
    theirs = lax.dot_general(hidden[half:], down_serve[0], dims, preferred_element_type=jnp.float32)
    arrived = lax.ppermute(theirs.astype(jnp.bfloat16), "c", [(0, 1), (1, 0)])
    mine = lax.dot_general(hidden[:half], down_serve[0], dims, preferred_element_type=jnp.float32)
    chip = (mine + arrived.astype(jnp.float32)).astype(jnp.bfloat16)
    chip = chip.reshape(NX, NZ * 2, width)
    by_x = lax.all_to_all(chip, "x", 0, 0, tiled=True).astype(jnp.float32).sum(axis=0)
    by_x = by_x.astype(jnp.bfloat16).reshape(NZ, 2, width)
    by_z = lax.all_to_all(by_x, "z", 0, 0, tiled=True).astype(jnp.float32).sum(axis=0)
    return (gate_serve, up_serve, down_serve, by_z.astype(jnp.bfloat16))


def solution(mesh):
    finer = Mesh(mesh.devices.reshape(NZ, NX, NC, NY), FS_TP)
    in_specs = (
        P(FS_TP, None),
        P(FS_TP, None),
        P(FS_TP, None),
        P(FS),
        P(None, FS, "y"),
        P(None, FS, "y"),
        P(None, FS, "y"),
    )
    out_specs = (P(FS, None, None), P(FS, None, None), P(FS, None, None), P(FS_TP, None))
    return jax.shard_map(
        per_device, mesh=finer, in_specs=in_specs, out_specs=out_specs, check_vma=False
    )
```

```python
import jax
import jax.numpy as jnp
from jax import lax
from jax.experimental import pallas as pl
from jax.experimental.pallas import tpu as pltpu
from jax.sharding import Mesh
from jax.sharding import PartitionSpec as P


FS = ("z", "x", "c")
FS_TP = ("z", "x", "c", "y")
NZ, NX, NC, NY = 16, 4, 2, 4
XC = NX * NC
PAD = 128


def normalize(tokens):
    values = tokens.astype(jnp.float32)
    row_mean = jnp.mean(values, axis=-1, keepdims=True)
    centered = values - row_mean
    row_var = jnp.mean(centered * centered, axis=-1, keepdims=True)
    return (centered * lax.rsqrt(row_var + 1e-05)).astype(jnp.bfloat16)


def route_table(route_experts, route_logits, count):
    first = jax.nn.sigmoid(route_logits[:, 0] - route_logits[:, 1])
    second = jax.nn.sigmoid(route_logits[:, 1] - route_logits[:, 0])
    labels = jnp.arange(count, dtype=jnp.int32)
    table = first[:, None] * (route_experts[:, 0:1] == labels[None, :]).astype(jnp.float32)
    table = table + second[:, None] * (route_experts[:, 1:2] == labels[None, :]).astype(jnp.float32)
    return table.astype(jnp.bfloat16)


def shift(array, axis, by, size):
    return lax.ppermute(array, axis, [(i, (i + by) % size) for i in range(size)])


def swap_core(array):
    return lax.ppermute(array, "c", [(0, 1), (1, 0)])


def pack_kernel(x_ref, gain, gate, up, down, out):
    experts, block = gate.shape[0], out.shape[-1]
    depth = gain.shape[1]
    line = lax.broadcasted_iota(jnp.int32, (depth, depth), 0)
    lane = lax.broadcasted_iota(jnp.int32, (depth, depth), 1)
    wide = jnp.broadcast_to(gain[...], (depth, depth))
    scale = jnp.sum(jnp.where(line == lane, wide, 0.0), axis=1, keepdims=True)
    for y in range(NY):
        e = lax.rem(x_ref[0] + y, experts)
        for s in range(XC):
            cut = slice(s * block, (s + 1) * block)
            out[s, y, 0] = (scale * gate[e, :, cut]).astype(jnp.bfloat16)
            out[s, y, 1] = (scale * up[e, :, cut]).astype(jnp.bfloat16)
            out[s, y, 2] = down[e, :, cut].astype(jnp.bfloat16)


def sort_kernel(y_ref, swapped, riders, early, late):
    depth = swapped.shape[3]
    for e in range(NZ // NY):
        x = lax.rem(NX + e - y_ref[0], NX)
        for y in range(NY):
            for c in range(NC):
                part = swapped[NC * x + c, y]
                early[NY * e + y, depth * c : depth * (c + 1)] = part[0]
                early[NY * e + y, depth * (NC + c) : depth * (NC + c + 1)] = part[1]
                late[NY * e + y, depth * c : depth * (c + 1)] = part[2]
            early[NY * e + y, 2 * NC * depth :] = riders[...]


def put(first_ref, ins, outs):
    for k, part in enumerate(ins):
        at = lax.rem(first_ref[0] + k, NX)
        for m, out in enumerate(outs):
            span = out.shape[2]
            out[:, at] = part[:, m * span : (m + 1) * span]


def all_y(own):
    return [own] + [shift(own, "y", k, NY) for k in range(1, NY)]


def hidden_kernel(first_ref, expert_ref, *refs):
    parts, (here, there, gate, up, out, rows) = refs[:NY], refs[NY:]
    put(first_ref, parts, (gate, up))
    half = here.shape[0]
    rows[:half] = here[...]
    rows[half:] = there[...]
    width = gate.shape[0] * gate.shape[1] * gate.shape[2]
    table = rows[:, width:].astype(jnp.float32)
    lane = lax.broadcasted_iota(jnp.int32, table.shape, 1)
    weight = jnp.sum(jnp.where(lane == expert_ref[0], table, 0.0), axis=1, keepdims=True)
    x = rows[:, :width]
    g = jnp.dot(x, gate[...].reshape(width, -1), preferred_element_type=jnp.float32)
    u = jnp.dot(x, up[...].reshape(width, -1), preferred_element_type=jnp.float32)
    out[...] = (weight * (g / (1.0 + jnp.exp(-g))) * u).astype(jnp.bfloat16)


def down_kernel(first_ref, x_ref, *refs):
    parts, (hidden, down, theirs, mine) = refs[:NY], refs[NY:]
    put(first_ref, parts, (down,))
    full = down[...].reshape(-1, down.shape[3])
    half = hidden.shape[0] // 2
    dims = (((1,), (1,)), ((), ()))
    both = lax.dot_general(hidden[...], full, dims, preferred_element_type=jnp.float32)
    both = both.reshape(2, NX, half // NX, both.shape[1])
    for k in range(NX):
        to = lax.rem(NX + x_ref[0] - k, NX)
        mine[to] = both[0, k]
        theirs[to] = both[1, k].astype(jnp.bfloat16)


def per_device(tokens, route_experts, route_logits, norm_gain, gate_train, up_train, down_train):
    experts, depth, wide = gate_train.shape
    own_rows, width = tokens.shape
    block = wide // XC
    smem, vmem = pl.BlockSpec(memory_space=pltpu.SMEM), pl.BlockSpec(memory_space=pltpu.VMEM)
    y, x = lax.axis_index("y"), lax.axis_index("x")
    expert = lax.axis_index("z") // (NZ // experts)
    first_block = lax.rem(NX + expert - y, NX).reshape(1).astype(jnp.int32)
    expert, y, x = (i.reshape(1).astype(jnp.int32) for i in (expert, y, x))

    local = pl.pallas_call(
        pack_kernel,
        out_shape=jax.ShapeDtypeStruct((XC, NY, 3, depth, block), jnp.bfloat16),
        in_specs=[smem] + [vmem] * 4,
        out_specs=vmem,
    )(x, norm_gain[None, :], gate_train, up_train, down_train)
    swapped = lax.all_to_all(
        local.reshape(XC * NY, 3, depth, block), ("x", "c", "y"), 0, 0, tiled=True
    )

    normed = normalize(tokens)
    table = route_table(route_experts, route_logits, experts)
    spread = own_rows * width // block
    riders = jnp.concatenate(
        [
            normed.reshape(spread, block),
            jnp.pad(table, ((0, 8 - own_rows), (0, block - experts))),
        ]
    )
    span = NC * depth
    early, late = pl.pallas_call(
        sort_kernel,
        out_shape=[
            jax.ShapeDtypeStruct((NZ, 2 * span + spread + 8, block), jnp.bfloat16),
            jax.ShapeDtypeStruct((NZ, span, block), jnp.bfloat16),
        ],
        in_specs=[smem, vmem, vmem],
        out_specs=[vmem, vmem],
    )(y, swapped.reshape(XC, NY, 3, depth, block), riders)
    first = lax.all_to_all(early, "z", 0, 0, tiled=True)
    first, late = lax.optimization_barrier((first, late))
    second = lax.all_to_all(late, "z", 0, 0, tiled=True)

    cut = 2 * span
    parts = all_y(first[:, :cut])
    rows_z = first[:, cut : cut + spread].reshape(NZ * own_rows, width)
    table_z = first[:, cut + spread : cut + spread + own_rows, :PAD]
    rows_z = jnp.concatenate([rows_z, table_z.reshape(NZ * own_rows, PAD)], axis=1)
    rows_x = [rows_z] + [shift(rows_z, "x", k, NX) for k in range(1, NX)]
    rows_x = jnp.concatenate(rows_x)
    rows_c = swap_core(rows_x)
    placed = jax.ShapeDtypeStruct((NZ, NX, span, block), jnp.bfloat16)
    gate_serve, up_serve, hidden = pl.pallas_call(
        hidden_kernel,
        out_shape=[
            placed,
            placed,
            jax.ShapeDtypeStruct((2 * rows_x.shape[0], block), jnp.bfloat16),
        ],
        in_specs=[smem, smem] + [vmem] * (len(parts) + 2),
        out_specs=[vmem] * 3,
        scratch_shapes=[pltpu.VMEM((2 * rows_x.shape[0], width + PAD), jnp.bfloat16)],
    )(first_block, expert, *parts, rows_x, rows_c)

    parts = all_y(second)
    half = rows_x.shape[0]
    down_serve, theirs, mine = pl.pallas_call(
        down_kernel,
        out_shape=[
            placed,
            jax.ShapeDtypeStruct((NX, half // NX, width), jnp.bfloat16),
            jax.ShapeDtypeStruct((NX, half // NX, width), jnp.float32),
        ],
        in_specs=[smem, smem] + [vmem] * (len(parts) + 1),
        out_specs=[vmem] * 3,
    )(first_block, x, *parts, hidden)
    gate_serve, up_serve, down_serve = (
        matrix.reshape(1, width, block) for matrix in (gate_serve, up_serve, down_serve)
    )

    chip = (mine + swap_core(theirs).astype(jnp.float32)).astype(jnp.bfloat16)
    by_x = lax.all_to_all(chip, "x", 0, 0, tiled=True).astype(jnp.float32).sum(axis=0)
    by_x = by_x.astype(jnp.bfloat16).reshape(NZ, own_rows, width)
    by_z = lax.all_to_all(by_x, "z", 0, 0, tiled=True).astype(jnp.float32).sum(axis=0)
    return (gate_serve, up_serve, down_serve, by_z.astype(jnp.bfloat16))


def solution(mesh):
    finer = Mesh(mesh.devices.reshape(NZ, NX, NC, NY), FS_TP)
    in_specs = (
        P(FS_TP, None),
        P(FS_TP, None),
        P(FS_TP, None),
        P(FS),
        P(None, FS, "y"),
        P(None, FS, "y"),
        P(None, FS, "y"),
    )
    out_specs = (P(FS, None, None), P(FS, None, None), P(FS, None, None), P(FS_TP, None))
    return jax.shard_map(
        per_device, mesh=finer, in_specs=in_specs, out_specs=out_specs, check_vma=False
    )
```

```python
import jax
import jax.numpy as jnp
from jax import lax
from jax.experimental import pallas as pl
from jax.experimental.pallas import tpu as pltpu
from jax.sharding import Mesh
from jax.sharding import PartitionSpec as P


FS = ("z", "x", "c")
FS_TP = ("z", "x", "c", "y")
NZ, NX, NC, NY = 16, 4, 2, 4
XC = NX * NC
PAD = 128


def normalize(tokens):
    values = tokens.astype(jnp.float32)
    row_mean = jnp.mean(values, axis=-1, keepdims=True)
    centered = values - row_mean
    row_var = jnp.mean(centered * centered, axis=-1, keepdims=True)
    return (centered * lax.rsqrt(row_var + 1e-05)).astype(jnp.bfloat16)


def route_table(route_experts, route_logits, count):
    first = jax.nn.sigmoid(route_logits[:, 0] - route_logits[:, 1])
    second = jax.nn.sigmoid(route_logits[:, 1] - route_logits[:, 0])
    labels = jnp.arange(count, dtype=jnp.int32)
    table = first[:, None] * (route_experts[:, 0:1] == labels[None, :]).astype(jnp.float32)
    table = table + second[:, None] * (route_experts[:, 1:2] == labels[None, :]).astype(jnp.float32)
    return table.astype(jnp.bfloat16)


def shift(array, axis, by, size):
    return lax.ppermute(array, axis, [(i, (i + by) % size) for i in range(size)])


def swap_core(array):
    return lax.ppermute(array, "c", [(0, 1), (1, 0)])


def pack_kernel(x_ref, gain, gate, up, down, out):
    experts, block = gate.shape[0], out.shape[-1]
    depth = gain.shape[1]
    line = lax.broadcasted_iota(jnp.int32, (depth, depth), 0)
    lane = lax.broadcasted_iota(jnp.int32, (depth, depth), 1)
    wide = jnp.broadcast_to(gain[...], (depth, depth))
    scale = jnp.sum(jnp.where(line == lane, wide, 0.0), axis=1, keepdims=True)
    for y in range(NY):
        e = lax.rem(x_ref[0] + y, experts)
        for s in range(XC):
            cut = slice(s * block, (s + 1) * block)
            out[s, y, 0] = (scale * gate[e, :, cut]).astype(jnp.bfloat16)
            out[s, y, 1] = (scale * up[e, :, cut]).astype(jnp.bfloat16)
            out[s, y, 2] = down[e, :, cut].astype(jnp.bfloat16)


def sort_kernel(y_ref, swapped, riders, out):
    kinds, depth = swapped.shape[2:4]
    for e in range(NZ // NY):
        x = lax.rem(NX + e - y_ref[0], NX)
        for y in range(NY):
            at = 0
            for m in range(kinds):
                for c in range(NC):
                    out[NY * e + y, at : at + depth] = swapped[NC * x + c, y, m]
                    at += depth
            out[NY * e + y, at:] = riders[...]


def put(first_ref, ins, outs):
    for k, part in enumerate(ins):
        at = lax.rem(first_ref[0] + k, NX)
        for m, out in enumerate(outs):
            span = out.shape[2]
            out[:, at] = part[:, m * span : (m + 1) * span]


def all_from(own, axis, size):
    got = [own]
    for k in range(1, size):
        got.append(shift(own, axis, k, size))
    return got


def hidden_kernel(first_ref, expert_ref, *refs):
    parts, (here, there, gate, up, out, rows) = refs[:NY], refs[NY:]
    put(first_ref, parts, (gate, up))
    half = here.shape[0]
    rows[:half] = here[...]
    rows[half:] = there[...]
    width = gate.shape[0] * gate.shape[1] * gate.shape[2]
    table = rows[:, width:].astype(jnp.float32)
    lane = lax.broadcasted_iota(jnp.int32, table.shape, 1)
    weight = jnp.sum(jnp.where(lane == expert_ref[0], table, 0.0), axis=1, keepdims=True)
    x = rows[:, :width]
    g = jnp.dot(x, gate[...].reshape(width, -1), preferred_element_type=jnp.float32)
    u = jnp.dot(x, up[...].reshape(width, -1), preferred_element_type=jnp.float32)
    out[...] = (weight * (g / (1.0 + jnp.exp(-g))) * u).astype(jnp.bfloat16)


def down_kernel(first_ref, x_ref, *refs):
    parts, (hidden, down, theirs, mine) = refs[:NY], refs[NY:]
    put(first_ref, parts, (down,))
    full = down[...].reshape(-1, down.shape[3])
    half = hidden.shape[0] // 2
    dims = (((1,), (1,)), ((), ()))
    both = lax.dot_general(hidden[...], full, dims, preferred_element_type=jnp.float32)
    both = both.reshape(2, NX, half // NX, both.shape[1])
    for k in range(NX):
        to = lax.rem(NX + x_ref[0] - k, NX)
        mine[to] = both[0, k]
        theirs[to] = both[1, k].astype(jnp.bfloat16)


def on_core(kernel, scalars, arrays, outs, scratch=(), limit=None):
    smem, vmem = pl.BlockSpec(memory_space=pltpu.SMEM), pl.BlockSpec(memory_space=pltpu.VMEM)
    return pl.pallas_call(
        kernel,
        out_shape=outs,
        in_specs=[smem] * len(scalars) + [vmem] * len(arrays),
        out_specs=[vmem] * len(outs),
        scratch_shapes=scratch,
        compiler_params=pltpu.CompilerParams(vmem_limit_bytes=limit),
    )(*scalars, *arrays)


def held(array):
    return pltpu.with_memory_space_constraint(array, pltpu.VMEM)


def per_device(tokens, route_experts, route_logits, norm_gain, gate_train, up_train, down_train):
    experts, depth, wide = gate_train.shape
    own_rows, width = tokens.shape
    block = wide // XC
    y, x = lax.axis_index("y"), lax.axis_index("x")
    expert = lax.axis_index("z") // (NZ // experts)
    first_block = lax.rem(NX + expert - y, NX).reshape(1).astype(jnp.int32)
    expert, y, x = (i.reshape(1).astype(jnp.int32) for i in (expert, y, x))

    bf16, f32 = jnp.bfloat16, jnp.float32
    (local,) = on_core(
        pack_kernel,
        (x,),
        (norm_gain[None, :], gate_train, up_train, down_train),
        [pltpu.VMEM((XC, NY, 3, depth, block), bf16)],
    )
    swapped = lax.all_to_all(
        local.reshape(XC * NY, 3, depth, block), ("x", "c", "y"), 0, 0, tiled=True
    )

    normed = normalize(tokens)
    table = route_table(route_experts, route_logits, experts)
    spread = own_rows * width // block
    riders = jnp.concatenate(
        [
            normed.reshape(spread, block),
            jnp.pad(table, ((0, 8 - own_rows), (0, block - experts))),
        ]
    )
    span = NC * depth
    cut = 3 * span
    (sorted_by_z,) = on_core(
        sort_kernel,
        (y,),
        (held(swapped.reshape(XC, NY, 3, depth, block)), held(riders)),
        [pltpu.VMEM((NZ, cut + spread + 8, block), bf16)],
        limit=8 << 20,
    )
    first = lax.all_to_all(sorted_by_z, "z", 0, 0, tiled=True)

    parts = all_from(first[:, : 2 * span], "y", NY)
    rows_z = first[:, cut : cut + spread].reshape(NZ * own_rows, width)
    table_z = first[:, cut + spread : cut + spread + own_rows, :PAD]
    rows_z = jnp.concatenate([rows_z, table_z.reshape(NZ * own_rows, PAD)], axis=1)
    rows_x = all_from(rows_z, "x", NX)
    rows_x = jnp.concatenate(rows_x)
    rows_c = swap_core(rows_x)
    placed = jax.ShapeDtypeStruct((NZ, NX, span, block), bf16)
    half = rows_x.shape[0]
    gate_serve, up_serve, hidden = on_core(
        hidden_kernel,
        (first_block, expert),
        (*parts, rows_x, rows_c),
        [placed, placed, pltpu.VMEM((2 * half, block), bf16)],
        [pltpu.VMEM((2 * half, width + PAD), bf16)],
    )

    parts = all_from(first[:, 2 * span : cut], "y", NY)
    down_serve, theirs, mine = on_core(
        down_kernel,
        (first_block, x),
        [held(a) for a in (*parts, hidden)],
        [
            placed,
            pltpu.VMEM((NX, half // NX, width), bf16),
            pltpu.VMEM((NX, half // NX, width), f32),
        ],
        limit=16 << 20,
    )
    gate_serve, up_serve, down_serve = (
        matrix.reshape(1, width, block) for matrix in (gate_serve, up_serve, down_serve)
    )

    chip = (mine + swap_core(theirs).astype(jnp.float32)).astype(jnp.bfloat16)
    by_x = lax.all_to_all(chip, "x", 0, 0, tiled=True).astype(jnp.float32).sum(axis=0)
    by_x = by_x.astype(jnp.bfloat16).reshape(NZ, own_rows, width)
    by_z = lax.all_to_all(by_x, "z", 0, 0, tiled=True).astype(jnp.float32).sum(axis=0)
    return (gate_serve, up_serve, down_serve, by_z.astype(jnp.bfloat16))


def solution(mesh):
    finer = Mesh(mesh.devices.reshape(NZ, NX, NC, NY), FS_TP)
    in_specs = (
        P(FS_TP, None),
        P(FS_TP, None),
        P(FS_TP, None),
        P(FS),
        P(None, FS, "y"),
        P(None, FS, "y"),
        P(None, FS, "y"),
    )
    out_specs = (P(FS, None, None), P(FS, None, None), P(FS, None, None), P(FS_TP, None))
    return jax.shard_map(
        per_device, mesh=finer, in_specs=in_specs, out_specs=out_specs, check_vma=False
    )
```

```python
import jax
import jax.numpy as jnp
from jax import lax
from jax.experimental import pallas as pl
from jax.experimental.pallas import tpu as pltpu
from jax.sharding import Mesh
from jax.sharding import PartitionSpec as P


FS = ("z", "x", "c")
FS_TP = ("z", "x", "c", "y")
NZ, NX, NC, NY = 16, 4, 2, 4
XC = NX * NC
LANES = 128
PAD = 128


def normalize(tokens):
    values = tokens.astype(jnp.float32)
    row_mean = jnp.mean(values, axis=-1, keepdims=True)
    centered = values - row_mean
    row_var = jnp.mean(centered * centered, axis=-1, keepdims=True)
    return (centered * lax.rsqrt(row_var + 1e-05)).astype(jnp.bfloat16)


def route_table(route_experts, route_logits, count):
    first = jax.nn.sigmoid(route_logits[:, 0] - route_logits[:, 1])
    second = jax.nn.sigmoid(route_logits[:, 1] - route_logits[:, 0])
    labels = jnp.arange(count, dtype=jnp.int32)
    table = first[:, None] * (route_experts[:, 0:1] == labels[None, :]).astype(jnp.float32)
    table = table + second[:, None] * (route_experts[:, 1:2] == labels[None, :]).astype(jnp.float32)
    return table.astype(jnp.bfloat16)


def shift(array, axis, by, size):
    return lax.ppermute(array, axis, [(i, (i + by) % size) for i in range(size)])


def swap_core(array):
    return lax.ppermute(array, "c", [(0, 1), (1, 0)])


def pack_kernel(x_ref, gain, gate, up, down, out):
    experts, block = gate.shape[0], out.shape[-1]
    depth = gain.shape[1]
    line = lax.broadcasted_iota(jnp.int32, (depth, depth), 0)
    lane = lax.broadcasted_iota(jnp.int32, (depth, depth), 1)
    wide = jnp.broadcast_to(gain[...], (depth, depth))
    scale = jnp.sum(jnp.where(line == lane, wide, 0.0), axis=1, keepdims=True)
    for y in range(NY):
        e = lax.rem(x_ref[0] + y, experts)
        for s in range(XC):
            cut = slice(s * block, (s + 1) * block)
            out[s, y, 0] = (scale * gate[e, :, cut]).astype(jnp.bfloat16)
            out[s, y, 1] = (scale * up[e, :, cut]).astype(jnp.bfloat16)
            out[s, y, 2] = down[e, :, cut].astype(jnp.bfloat16)


def sort_kernel(y_ref, swapped, riders, out):
    kinds, depth, wide = swapped.shape[2:]
    for e in range(NZ // NY):
        x = lax.rem(NX + e - y_ref[0], NX)
        for y in range(NY):
            at = 0
            for m in range(kinds):
                for lane in range(0, wide, LANES):
                    for c in range(NC):
                        part = swapped[NC * x + c, y, m, :, lane : lane + LANES]
                        out[NY * e + y, at : at + depth] = part
                        at += depth
            out[NY * e + y, at:] = riders[...]


def put(first_ref, ins, outs):
    for k, part in enumerate(ins):
        at, row = lax.rem(first_ref[0] + k, NX), 0
        for out in outs:
            span, wide = out.shape[2:]
            for lane in range(0, wide, LANES):
                out[:, at, :, lane : lane + LANES] = part[:, row : row + span]
                row += span


def all_from(own, axis, size):
    got = [own]
    for k in range(1, size):
        got.append(shift(own, axis, k, size))
    return got


def hidden_kernel(first_ref, expert_ref, *refs):
    parts, (rows, gate, up, out) = refs[:NY], refs[NY:]
    put(first_ref, parts, (gate, up))
    width = gate.shape[0] * gate.shape[1] * gate.shape[2]
    table = rows[:, width:].astype(jnp.float32)
    lane = lax.broadcasted_iota(jnp.int32, table.shape, 1)
    weight = jnp.sum(jnp.where(lane == expert_ref[0], table, 0.0), axis=1, keepdims=True)
    x = rows[:, :width]
    g = jnp.dot(x, gate[...].reshape(width, -1), preferred_element_type=jnp.float32)
    u = jnp.dot(x, up[...].reshape(width, -1), preferred_element_type=jnp.float32)
    hidden = (weight * (g / (1.0 + jnp.exp(-g))) * u).astype(jnp.bfloat16)
    out[...] = hidden.reshape(out.shape)


def down_kernel(first_ref, c_ref, *refs):
    parts, (hidden, down, theirs, mine) = refs[:NY], refs[NY:]
    put(first_ref, parts, (down,))
    full = down[...].reshape(-1, down.shape[3])
    dims = (((1,), (1,)), ((), ()))
    for out, core in ((theirs, 1 - c_ref[0]), (mine, c_ref[0])):
        act = hidden[:, core].reshape(-1, full.shape[1])
        got = lax.dot_general(act, full, dims, preferred_element_type=jnp.float32)
        out[...] = got.reshape(out.shape).astype(out.dtype)


def on_core(kernel, scalars, arrays, outs, scratch=(), limit=None):
    smem, vmem = pl.BlockSpec(memory_space=pltpu.SMEM), pl.BlockSpec(memory_space=pltpu.VMEM)
    return pl.pallas_call(
        kernel,
        out_shape=outs,
        in_specs=[smem] * len(scalars) + [vmem] * len(arrays),
        out_specs=[vmem] * len(outs),
        scratch_shapes=scratch,
        compiler_params=pltpu.CompilerParams(vmem_limit_bytes=limit),
    )(*scalars, *arrays)


def held(array):
    return pltpu.with_memory_space_constraint(array, pltpu.VMEM)


def per_device(tokens, route_experts, route_logits, norm_gain, gate_train, up_train, down_train):
    experts, depth, wide = gate_train.shape
    own_rows, width = tokens.shape
    block = wide // XC
    y, x, c = (lax.axis_index(axis) for axis in ("y", "x", "c"))
    expert = lax.axis_index("z") // (NZ // experts)
    first_block = lax.rem(NX + expert - y, NX).reshape(1).astype(jnp.int32)
    expert, y, x, c = (i.reshape(1).astype(jnp.int32) for i in (expert, y, x, c))

    bf16, f32 = jnp.bfloat16, jnp.float32
    (local,) = on_core(
        pack_kernel,
        (x,),
        (norm_gain[None, :], gate_train, up_train, down_train),
        [pltpu.VMEM((XC, NY, 3, depth, block), bf16)],
    )
    swapped = lax.all_to_all(
        local.reshape(XC * NY, 3, depth, block), ("x", "c", "y"), 0, 0, tiled=True
    )

    normed = normalize(tokens)
    table = route_table(route_experts, route_logits, experts)
    spread = own_rows * width // LANES
    riders = jnp.concatenate(
        [
            normed.reshape(spread, LANES),
            jnp.pad(table, ((0, 8 - own_rows), (0, LANES - experts))),
        ]
    )
    span = NC * depth
    one = span * (block // LANES)
    cut = 3 * one
    (sorted_by_z,) = on_core(
        sort_kernel,
        (y,),
        (held(swapped.reshape(XC, NY, 3, depth, block)), held(riders)),
        [pltpu.VMEM((NZ, cut + spread + 8, LANES), bf16)],
        limit=8 << 20,
    )
    first = lax.all_to_all(sorted_by_z, "z", 0, 0, tiled=True)

    parts = all_from(first[:, : 2 * one], "y", NY)
    rows_z = first[:, cut : cut + spread].reshape(NZ * own_rows, width)
    table_z = first[:, cut + spread : cut + spread + own_rows]
    rows_z = jnp.concatenate([rows_z, table_z.reshape(NZ * own_rows, PAD)], axis=1)
    copies = jnp.broadcast_to(rows_z[None], (XC, *rows_z.shape))
    rows_all = lax.all_to_all(copies, ("x", "c"), 0, 0, tiled=True)
    rows_all = rows_all.reshape(-1, width + PAD)
    placed = jax.ShapeDtypeStruct((NZ, NX, span, block), bf16)
    count = rows_all.shape[0]
    gate_serve, up_serve, hidden = on_core(
        hidden_kernel,
        (first_block, expert),
        [held(a) for a in (*parts, rows_all)],
        [placed, placed, pltpu.VMEM((NX, NC, count // XC, block), bf16)],
        limit=16 << 20,
    )

    parts = all_from(first[:, 2 * one : cut], "y", NY)
    down_serve, theirs, mine = on_core(
        down_kernel,
        (first_block, c),
        [held(a) for a in (*parts, hidden)],
        [
            placed,
            pltpu.VMEM((NX, count // XC, width), bf16),
            pltpu.VMEM((NX, count // XC, width), f32),
        ],
        limit=16 << 20,
    )
    gate_serve, up_serve, down_serve = (
        matrix.reshape(1, width, block) for matrix in (gate_serve, up_serve, down_serve)
    )

    chip = (mine + swap_core(theirs).astype(jnp.float32)).astype(jnp.bfloat16)
    by_x = lax.all_to_all(chip, "x", 0, 0, tiled=True).astype(jnp.float32).sum(axis=0)
    by_x = by_x.astype(jnp.bfloat16).reshape(NZ, own_rows, width)
    by_z = lax.all_to_all(by_x, "z", 0, 0, tiled=True).astype(jnp.float32).sum(axis=0)
    return (gate_serve, up_serve, down_serve, by_z.astype(jnp.bfloat16))


def solution(mesh):
    finer = Mesh(mesh.devices.reshape(NZ, NX, NC, NY), FS_TP)
    in_specs = (
        P(FS_TP, None),
        P(FS_TP, None),
        P(FS_TP, None),
        P(FS),
        P(None, FS, "y"),
        P(None, FS, "y"),
        P(None, FS, "y"),
    )
    out_specs = (P(FS, None, None), P(FS, None, None), P(FS, None, None), P(FS_TP, None))
    return jax.shard_map(
        per_device, mesh=finer, in_specs=in_specs, out_specs=out_specs, check_vma=False
    )
```

```python
import jax
import jax.numpy as jnp
from jax import lax
from jax.experimental import pallas as pl
from jax.experimental.pallas import tpu as pltpu
from jax.sharding import Mesh
from jax.sharding import PartitionSpec as P


FS = ("z", "x", "c")
FS_TP = ("z", "x", "c", "y")
NZ, NX, NC, NY = 16, 4, 2, 4
XC = NX * NC
LANES = 128
PAD = 128


def normalize(tokens):
    values = tokens.astype(jnp.float32)
    row_mean = jnp.mean(values, axis=-1, keepdims=True)
    centered = values - row_mean
    row_var = jnp.mean(centered * centered, axis=-1, keepdims=True)
    return (centered * lax.rsqrt(row_var + 1e-05)).astype(jnp.bfloat16)


def route_table(route_experts, route_logits, count):
    first = jax.nn.sigmoid(route_logits[:, 0] - route_logits[:, 1])
    second = jax.nn.sigmoid(route_logits[:, 1] - route_logits[:, 0])
    labels = jnp.arange(count, dtype=jnp.int32)
    table = first[:, None] * (route_experts[:, 0:1] == labels[None, :]).astype(jnp.float32)
    table = table + second[:, None] * (route_experts[:, 1:2] == labels[None, :]).astype(jnp.float32)
    return table.astype(jnp.bfloat16)


def shift(array, axis, by, size):
    return lax.ppermute(array, axis, [(i, (i + by) % size) for i in range(size)])


def swap_core(array):
    return lax.ppermute(array, "c", [(0, 1), (1, 0)])


def pack_kernel(x_ref, gain, gate, up, down, out):
    experts, block = gate.shape[0], out.shape[-1]
    depth = gain.shape[1]
    line = lax.broadcasted_iota(jnp.int32, (depth, depth), 0)
    lane = lax.broadcasted_iota(jnp.int32, (depth, depth), 1)
    wide = jnp.broadcast_to(gain[...], (depth, depth))
    scale = jnp.sum(jnp.where(line == lane, wide, 0.0), axis=1, keepdims=True)
    for y in range(NY):
        e = lax.rem(x_ref[0] + y, experts)
        for s in range(XC):
            cut = slice(s * block, (s + 1) * block)
            out[s, y, 0] = (scale * gate[e, :, cut]).astype(jnp.bfloat16)
            out[s, y, 1] = (scale * up[e, :, cut]).astype(jnp.bfloat16)
            out[s, y, 2] = down[e, :, cut].astype(jnp.bfloat16)


def sort_kernel(y_ref, swapped, riders, out):
    kinds, depth, wide = swapped.shape[2:]
    for e in range(NZ // NY):
        x = lax.rem(NX + e - y_ref[0], NX)
        for y in range(NY):
            at = 0
            for m in range(kinds):
                for lane in range(0, wide, LANES):
                    for c in range(NC):
                        part = swapped[NC * x + c, y, m, :, lane : lane + LANES]
                        out[NY * e + y, at : at + depth] = part
                        at += depth
            out[NY * e + y, at:] = riders[...]


def put(first_ref, ins, outs):
    for k, part in enumerate(ins):
        at, row = lax.rem(first_ref[0] + k, NX), 0
        for out in outs:
            span, wide = out.shape[2:]
            cuts = range(row, row + span * (wide // LANES), span)
            out[:, at] = jnp.concatenate([part[:, i : i + span] for i in cuts], axis=2)
            row = cuts.stop


def all_from(own, axis, size):
    got = [own]
    for k in range(1, size):
        got.append(shift(own, axis, k, size))
    return got


def hidden_kernel(first_ref, expert_ref, *refs):
    parts, (rows, gate, up, out) = refs[:NY], refs[NY:]
    put(first_ref, parts, (gate, up))
    width = gate.shape[0] * gate.shape[1] * gate.shape[2]
    table = rows[:, width:].astype(jnp.float32)
    lane = lax.broadcasted_iota(jnp.int32, table.shape, 1)
    weight = jnp.sum(jnp.where(lane == expert_ref[0], table, 0.0), axis=1, keepdims=True)
    x = rows[:, :width]
    g = jnp.dot(x, gate[...].reshape(width, -1), preferred_element_type=jnp.float32)
    u = jnp.dot(x, up[...].reshape(width, -1), preferred_element_type=jnp.float32)
    hidden = (weight * (g / (1.0 + jnp.exp(-g))) * u).astype(jnp.bfloat16)
    out[...] = hidden.reshape(out.shape)


def product(core, hidden, down, out):
    full = down[...].reshape(-1, down.shape[3])
    act = hidden[:, core].reshape(-1, full.shape[1])
    dims = (((1,), (1,)), ((), ()))
    got = lax.dot_general(act, full, dims, preferred_element_type=jnp.float32)
    out[...] = got.reshape(out.shape).astype(out.dtype)


def theirs_kernel(first_ref, c_ref, *refs):
    parts, (hidden, down, theirs) = refs[:NY], refs[NY:]
    put(first_ref, parts, (down,))
    product(1 - c_ref[0], hidden, down, theirs)


def mine_kernel(c_ref, hidden, down, mine):
    product(c_ref[0], hidden, down, mine)


def on_core(kernel, scalars, arrays, outs, scratch=(), limit=None):
    smem, vmem = pl.BlockSpec(memory_space=pltpu.SMEM), pl.BlockSpec(memory_space=pltpu.VMEM)
    return pl.pallas_call(
        kernel,
        out_shape=outs,
        in_specs=[smem] * len(scalars) + [vmem] * len(arrays),
        out_specs=[vmem] * len(outs),
        scratch_shapes=scratch,
        compiler_params=pltpu.CompilerParams(vmem_limit_bytes=limit),
    )(*scalars, *arrays)


def held(array):
    return pltpu.with_memory_space_constraint(array, pltpu.VMEM)


def per_device(tokens, route_experts, route_logits, norm_gain, gate_train, up_train, down_train):
    experts, depth, wide = gate_train.shape
    own_rows, width = tokens.shape
    block = wide // XC
    y, x, c = (lax.axis_index(axis) for axis in ("y", "x", "c"))
    expert = lax.axis_index("z") // (NZ // experts)
    first_block = lax.rem(NX + expert - y, NX).reshape(1).astype(jnp.int32)
    expert, y, x, c = (i.reshape(1).astype(jnp.int32) for i in (expert, y, x, c))

    bf16, f32 = jnp.bfloat16, jnp.float32
    (local,) = on_core(
        pack_kernel,
        (x,),
        (norm_gain[None, :], gate_train, up_train, down_train),
        [pltpu.VMEM((XC, NY, 3, depth, block), bf16)],
    )
    swapped = lax.all_to_all(
        local.reshape(XC * NY, 3, depth, block), ("x", "c", "y"), 0, 0, tiled=True
    )

    normed = normalize(tokens)
    table = route_table(route_experts, route_logits, experts)
    spread = own_rows * width // LANES
    riders = jnp.concatenate(
        [
            normed.reshape(spread, LANES),
            jnp.pad(table, ((0, 8 - own_rows), (0, LANES - experts))),
        ]
    )
    span = NC * depth
    one = span * (block // LANES)
    cut = 3 * one
    (sorted_by_z,) = on_core(
        sort_kernel,
        (y,),
        (held(swapped.reshape(XC, NY, 3, depth, block)), held(riders)),
        [pltpu.VMEM((NZ, cut + spread + 8, LANES), bf16)],
        limit=8 << 20,
    )
    first = lax.all_to_all(sorted_by_z, "z", 0, 0, tiled=True)

    parts = all_from(first[:, : 2 * one], "y", NY)
    rows_z = first[:, cut : cut + spread].reshape(NZ * own_rows, width)
    table_z = first[:, cut + spread : cut + spread + own_rows]
    rows_z = jnp.concatenate([rows_z, table_z.reshape(NZ * own_rows, PAD)], axis=1)
    copies = jnp.broadcast_to(rows_z[None], (XC, *rows_z.shape))
    rows_all = lax.all_to_all(copies, ("x", "c"), 0, 0, tiled=True)
    rows_all = rows_all.reshape(-1, width + PAD)
    placed = jax.ShapeDtypeStruct((NZ, NX, span, block), bf16)
    count = rows_all.shape[0]
    gate_serve, up_serve, hidden = on_core(
        hidden_kernel,
        (first_block, expert),
        [held(a) for a in (*parts, rows_all)],
        [placed, placed, pltpu.VMEM((NX, NC, count // XC, block), bf16)],
        limit=16 << 20,
    )

    parts = all_from(first[:, 2 * one : cut], "y", NY)
    hidden = held(hidden)
    down_serve, theirs = on_core(
        theirs_kernel,
        (first_block, c),
        (*[held(a) for a in parts], hidden),
        [pltpu.VMEM(placed.shape, bf16), pltpu.VMEM((NX, count // XC, width), bf16)],
        limit=16 << 20,
    )
    arrived = swap_core(theirs)
    (mine,) = on_core(
        mine_kernel,
        (c,),
        (hidden, held(down_serve)),
        [pltpu.VMEM((NX, count // XC, width), f32)],
        limit=16 << 20,
    )
    gate_serve, up_serve, down_serve = (
        matrix.reshape(1, width, block) for matrix in (gate_serve, up_serve, down_serve)
    )

    chip = (mine + arrived.astype(jnp.float32)).astype(jnp.bfloat16)
    by_x = lax.all_to_all(chip, "x", 0, 0, tiled=True).astype(jnp.float32).sum(axis=0)
    by_x = by_x.astype(jnp.bfloat16).reshape(NZ, own_rows, width)
    by_z = lax.all_to_all(by_x, "z", 0, 0, tiled=True).astype(jnp.float32).sum(axis=0)
    return (gate_serve, up_serve, down_serve, by_z.astype(jnp.bfloat16))


def solution(mesh):
    finer = Mesh(mesh.devices.reshape(NZ, NX, NC, NY), FS_TP)
    in_specs = (
        P(FS_TP, None),
        P(FS_TP, None),
        P(FS_TP, None),
        P(FS),
        P(None, FS, "y"),
        P(None, FS, "y"),
        P(None, FS, "y"),
    )
    out_specs = (P(FS, None, None), P(FS, None, None), P(FS, None, None), P(FS_TP, None))
    return jax.shard_map(
        per_device, mesh=finer, in_specs=in_specs, out_specs=out_specs, check_vma=False
    )
```
